512 devices in a mesh: sp: 64 (over z, y), fs: 4 (over x), tp: 2 (over core).
Axes of the slice: x: 4, y: 8, z: 8, core: 2. Of those that a mesh axis runs over, the one named last changes fastest.
Arguments:
- tokens: bfloat16 [12288, 4096], P('sp', ('fs', 'tp')), may hold values from -6 to 6
- norm_gain: float32 [4096], replicated, may hold values from 0.1 to 1.9
- w_conv_in: bfloat16 [4096, 1024], P('sp', ('fs', 'tp')), may hold values from -0.09375 to 0.09375
- w_conv_b: bfloat16 [4096, 1024], P('sp', ('fs', 'tp')), may hold values from -0.09375 to 0.09375
- w_conv_c: bfloat16 [4096, 1024], P('sp', ('fs', 'tp')), may hold values from -0.09375 to 0.09375
- conv_taps: float32 [3, 1024], P(None, ('fs', 'tp')), may hold values from -1.2 to 1.2
- w_query: bfloat16 [4096, 2048], P('sp', ('fs', 'tp')), may hold values from -1 to 1
- w_key: bfloat16 [4096, 2048], P('sp', ('fs', 'tp')), may hold values from -1 to 1
- w_value: bfloat16 [4096, 2048], P('sp', ('fs', 'tp')), may hold values from -0.09375 to 0.09375
- lam: float32 [8], P(('fs', 'tp')), may hold values from 0.3 to 0.8
- head_scale: float32 [8, 256], P(('fs', 'tp')), may hold values from 0.2 to 3.5
- gain_conv: float32 [1024], P(('fs', 'tp')), may hold values from 0.1 to 1.9
- gain_attn: float32 [2048], P(('fs', 'tp')), may hold values from 0.1 to 1.9
Outputs:
- conv_mixed: float32 [12288, 1024], P('sp', ('fs', 'tp'))
- attn_mixed: float32 [12288, 2048], P('sp', ('fs', 'tp'))
The draws below stay inside these ranges and needn't reach their ends.
All inputs are finite; a program needn't handle non-finite values.
Results may differ from the reference program's by a relative error of at most 0.012.
The reference program's roundings to bfloat16 on the way count: a program that leaves them out, or rounds other values in their place, can miss the bound.
Values may be sent and summed in bfloat16 or wider, within the bound.
A program may use at most 128 MiB of HBM per device.

```python
import math
import jax
import jax.numpy as jnp
from jax import lax

D = 4096
CH = 1024
HEADS = 8
DK = 128
DV = 256
BLOCK = 64
TOK_DEV = 192
LENGTH = 12288
TOKENS = 12288


def draw_tokens(key, part):
    base = jax.random.normal(jax.random.fold_in(key, 11), (TOKENS, D), jnp.float32)
    return jnp.clip(base, -6.0, 6.0).astype(jnp.bfloat16)


def draw_w_query(key, part):
    matrix = jax.random.normal(jax.random.fold_in(key, 21), (D, HEADS * 2 * DK), jnp.float32) * (1.4 / math.sqrt(D))
    return jnp.clip(matrix, -1.0, 1.0).astype(jnp.bfloat16)


def draw_w_key(key, part):
    matrix = jax.random.normal(jax.random.fold_in(key, 22), (D, HEADS * 2 * DK), jnp.float32) * (1.4 / math.sqrt(D))
    return jnp.clip(matrix, -1.0, 1.0).astype(jnp.bfloat16)


def draw_head_scale(key, part):
    per_head = jnp.exp(jax.random.uniform(jax.random.fold_in(key, 31), (HEADS, 1), jnp.float32, math.log(0.3), math.log(3.0)))
    spread = 1.0 + 0.15 * jax.random.uniform(jax.random.fold_in(key, 32), (HEADS, DV), jnp.float32, -1.0, 1.0)
    return (per_head * spread).astype(jnp.float32)


def draw_conv_taps(key, part):
    sizes = jax.random.uniform(jax.random.fold_in(key, 41), (3, CH), jnp.float32, 0.6, 1.2)
    sizes = sizes * jnp.array([1.0, 1.0, 0.45], jnp.float32)[:, None]
    signs = jnp.where(jax.random.bernoulli(jax.random.fold_in(key, 42), 0.5, (3, CH)), 1.0, -1.0)
    return (sizes * signs).astype(jnp.float32)


def shard_levels(stream_key, shape, pieces, least, top_value):
    loudness = 1.0
    for position, parts in pieces:
        draws = jax.random.uniform(jax.random.fold_in(jax.random.fold_in(stream_key, 6), position), (parts,), jnp.float32, least / len(pieces), top_value / len(pieces))
        loudness = loudness * jnp.repeat(jnp.exp(draws), shape[position] // parts).reshape((-1,) + (1,) * (len(shape) - 1 - position))
    return loudness


def gaussian(key, dims, width, reach, cuts=(), held_as=jnp.bfloat16):
    entries = width * jax.random.normal(key, dims, jnp.float32)
    if cuts:
        entries = entries * shard_levels(key, dims, cuts, -0.22, 0.18)
    return jnp.clip(entries, -reach, reach).astype(held_as)


def setup_inputs(seed: int = 0) -> dict:
    key_list = jax.random.split(jax.random.key(seed), 14)
    tokens = draw_tokens(jax.random.fold_in(key_list[13], 71), 0)
    norm_gain = jnp.clip(1.0 + 0.18 * jax.random.normal(key_list[1], (D,), jnp.float32), 0.1, 1.9)
    w_conv_in = gaussian(key_list[2], (D, CH), D ** -0.5, 0.09375, ((0, 64), (1, 8)))
    w_conv_b = gaussian(key_list[3], (D, CH), D ** -0.5, 0.09375, ((0, 64), (1, 8)))
    w_conv_c = gaussian(key_list[4], (D, CH), D ** -0.5, 0.09375, ((0, 64), (1, 8)))
    conv_taps = draw_conv_taps(jax.random.fold_in(key_list[13], 71), 0)
    w_query = draw_w_query(jax.random.fold_in(key_list[13], 71), 0)
    w_key = draw_w_key(jax.random.fold_in(key_list[13], 71), 0)
    w_value = gaussian(key_list[8], (D, HEADS * DV), D ** -0.5, 0.09375, ((0, 64), (1, 8)))
    lam = jnp.clip(0.3 + 0.5 * jax.random.uniform(key_list[9], (HEADS,), jnp.float32) ** shard_levels(key_list[9], (HEADS,), ((0, 8),), -0.2, 0.2), 0.3, 0.8)
    head_scale = draw_head_scale(jax.random.fold_in(key_list[13], 71), 0)
    gain_conv = jnp.clip(1.0 + 0.18 * jax.random.normal(key_list[11], (CH,), jnp.float32), 0.1, 1.9)
    gain_attn = jnp.clip(1.0 + 0.18 * jax.random.normal(key_list[12], (HEADS * DV,), jnp.float32), 0.1, 1.9)
    return {"tokens": tokens, "norm_gain": norm_gain, "w_conv_in": w_conv_in, "w_conv_b": w_conv_b, "w_conv_c": w_conv_c, "conv_taps": conv_taps, "w_query": w_query, "w_key": w_key, "w_value": w_value, "lam": lam, "head_scale": head_scale, "gain_conv": gain_conv, "gain_attn": gain_attn}


EPS = 1e-06
masked_score = -1e+30

def reference(tokens, norm_gain, w_conv_in, w_conv_b, w_conv_c, conv_taps, w_query, w_key, w_value, lam, head_scale, gain_conv, gain_attn):
    values_in = tokens.astype(jnp.float32)
    normed = (values_in * lax.rsqrt(lax.optimization_barrier(jnp.mean(values_in * values_in, axis=-1, keepdims=True)) + EPS) * norm_gain).astype(jnp.bfloat16)

    def project(weight):
        return jnp.dot(normed, weight, preferred_element_type=jnp.float32).astype(jnp.bfloat16)
    conv_in = project(w_conv_in)
    conv_b = project(w_conv_b)
    conv_c = project(w_conv_c)
    mixed_in = (conv_c.astype(jnp.float32) * conv_in.astype(jnp.float32)).astype(jnp.bfloat16)
    mixed_in = lax.optimization_barrier(mixed_in).astype(jnp.float32)
    sequences = TOKENS // LENGTH
    shaped = mixed_in.reshape(sequences, LENGTH, CH)
    padded = jnp.pad(shaped, ((0, 0), (2, 0), (0, 0)))
    convolved = conv_taps[0] * padded[:, :LENGTH] + conv_taps[1] * padded[:, 1:LENGTH + 1] + conv_taps[2] * padded[:, 2:]
    conv_out = conv_b.astype(jnp.float32) * convolved.reshape(TOKENS, CH)
    queries = project(w_query).reshape(sequences, LENGTH, HEADS, 2, DK)
    keys_all = project(w_key).reshape(sequences, LENGTH, HEADS, 2, DK)
    values_all = project(w_value).reshape(sequences, LENGTH, HEADS, DV)
    blocks_per = LENGTH // TOK_DEV

    def one_sequence(packed):
        seq_queries, seq_keys, seq_values = packed
        key_float = seq_keys.astype(jnp.float32)
        value_float = seq_values.astype(jnp.float32)
        query_blocks = seq_queries.reshape(blocks_per, TOK_DEV, HEADS, 2, DK)
        starts = jnp.arange(blocks_per, dtype=jnp.int32) * TOK_DEV
        key_pos = jnp.arange(LENGTH, dtype=jnp.int32)

        def one_block(pair):
            block_queries, start = pair
            query_pos = start + jnp.arange(TOK_DEV, dtype=jnp.int32)
            scores = jnp.einsum('qhcd,khcd->chqk', block_queries.astype(jnp.float32), key_float) * DK ** (-0.5)
            visible = key_pos[None, :] // BLOCK <= query_pos[:, None] // BLOCK
            scores = jnp.where(visible, scores, masked_score)
            row_max = lax.optimization_barrier(jnp.max(scores, axis=-1, keepdims=True))
            weights = jnp.where(visible, jnp.exp(scores - row_max), 0.0)
            denom = lax.optimization_barrier(jnp.sum(weights, axis=-1))
            rounded = lax.optimization_barrier(weights.astype(jnp.bfloat16)).astype(jnp.float32)
            readout = jnp.einsum('chqk,khd->chqd', rounded, value_float) / denom[..., None]
            difference = readout[0] - lam[:, None, None] * readout[1]
            headed = difference * lax.rsqrt(lax.optimization_barrier(jnp.mean(difference * difference, axis=-1, keepdims=True)) + EPS) * head_scale[:, None, :]
            return headed.transpose(1, 0, 2).reshape(TOK_DEV, HEADS * DV)
        return lax.map(one_block, (query_blocks, starts)).reshape(LENGTH, HEADS * DV)
    attn = lax.map(one_sequence, (queries, keys_all, values_all)).reshape(TOKENS, HEADS * DV)
    total = lax.optimization_barrier(jnp.sum(conv_out * conv_out, axis=1)) + lax.optimization_barrier(jnp.sum(attn * attn, axis=1))
    inv_rms = lax.rsqrt(total / (CH + HEADS * DV) + EPS)[:, None]
    conv_mixed = conv_out * inv_rms * gain_conv
    attn_mixed = attn * inv_rms * gain_attn
    return (conv_mixed, attn_mixed)
```

```python
import functools
import math

import jax
import jax.numpy as jnp
from jax import lax
from jax.experimental import pallas as pl
from jax.experimental.pallas import tpu as pltpu
from jax.sharding import PartitionSpec as P

NY = 8
NZ = 8
D = 4096
CH = 1024
HEADS = 8
DK = 128
DV = 256
ROWS = 192
UNIT = 64
EPS = 1e-06
MASKED = -1e30
LOG2E = 1.4426950408889634
LN2 = 0.6931471805599453
MESH = pl.DeviceIdType.MESH

COLS = 1152
PIECES = ((0, 256), (256, 256), (512, 256), (768, 384))


def rem(a, n):
    return lax.rem(a, jnp.int32(n))


def div(a, n):
    return lax.div(a, jnp.int32(n))


def to_row(column):
    wide = jnp.broadcast_to(column, (ROWS, 128))
    return jnp.transpose(wide)[0:8]


def to_column(row):
    tall = jnp.broadcast_to(row, (128, ROWS))
    return jnp.transpose(tall)[:, 0:1]


def kernel(
    tokens,
    w_key,
    w_value,
    w_query,
    w_conv_in,
    w_conv_b,
    w_conv_c,
    norm_gain,
    conv_taps,
    lam,
    head_scale,
    gain_conv,
    gain_attn,
    conv_ref,
    attn_ref,
    tok,
    wts,
    nrm,
    acc,
    keys,
    values,
    queries,
    mixed,
    halo,
    out_slots,
    out_rows,
    in_slots,
    in_rows,
    squares,
    conv_out,
    read,
    local_sem,
    tok_send,
    tok_recv,
    w_send,
    w_recv,
    k_send,
    k_recv,
    v_send,
    v_recv,
    q_send,
    q_recv,
    halo_send,
    halo_recv,
    o_send,
    o_recv,
    l_send,
    l_recv,
    s_send,
    s_recv,
):
    sp = lax.axis_index("sp")
    x = lax.axis_index("fs")
    core = lax.axis_index("tp")
    y = rem(sp, NY)
    z = div(sp, NY)
    mine = 2 * x + core

    def at(s, f=x, t=core):
        return (s, f, t)

    def along_y(d):
        return sp + rem(y + d + NY, NY) - y

    def along_z(d):
        return sp + (rem(z + d + NZ, NZ) - z) * NY

    def send(src, dst, send_sem, recv_sem, device):
        pltpu.make_async_remote_copy(
            src_ref=src,
            dst_ref=dst,
            send_sem=send_sem,
            recv_sem=recv_sem,
            device_id=device,
            device_id_type=MESH,
        ).start()

    def arrived(ref, sem):
        pltpu.make_async_copy(ref, ref, sem).wait()

    own = [
        pltpu.make_async_copy(tokens, tok.at[mine], local_sem.at[0]),
    ]
    start = 0
    for k, w in enumerate((w_key, w_value, w_query, w_conv_in, w_conv_b, w_conv_c)):
        width = w.shape[1]
        own.append(
            pltpu.make_async_copy(
                w, wts.at[sp, :, pl.ds(start, width)], local_sem.at[1 + k]
            )
        )
        start += width
    for copy in own:
        copy.start()

    barrier = pltpu.get_barrier_semaphore()

    def greet(device):
        pl.semaphore_signal(barrier, inc=1, device_id=device, device_id_type=MESH)

    for d in (1, -1):
        greet(at(along_y(d)))
        greet(at(along_z(d)))
    for k in range(1, 8):
        other = rem(mine + k, 8)
        greet((sp, div(other, 2), rem(other, 2)))
    before = rem(sp + NY * NZ - 1, NY * NZ)
    after = rem(sp + 1, NY * NZ)
    greet(at(before))
    for copy in own:
        copy.wait()
    pl.semaphore_wait(barrier, 12)

    for k in (1, 3, 2):
        send(
            tok.at[mine],
            tok.at[mine],
            tok_send,
            tok_recv.at[mine],
            at(sp, rem(x + k, 4)),
        )
    send(tok.at[mine], tok.at[mine], tok_send, tok_recv.at[mine], at(sp, x, 1 - core))

    stride1 = 1 + 7 * core
    stride2 = 8 - 7 * core
    pos1 = rem(lax.div(sp, stride1), 8)
    pos2 = rem(lax.div(sp, stride2), 8)

    def unit(d1, d2):
        return rem(pos1 + d1 + 8, 8) * stride1 + rem(pos2 + d2 + 8, 8) * stride2

    def pass_on(u, d1, d2):
        send(wts.at[u], wts.at[u], w_send, w_recv.at[u], at(unit(d1, d2)))

    def w_wait(u):
        arrived(wts.at[u], w_recv.at[u])

    def offset(j):
        return div(j + 1, 2) * (1 - 2 * rem(j, 2))

    def multiply(u):
        rows = nrm[u]
        for first, width in PIECES:
            cols = pl.ds(first, width)
            acc[:, cols] += jnp.dot(
                rows, wts[u, :, cols], preferred_element_type=jnp.float32
            )

    def first_ring(j, _):
        off = offset(j)
        u = unit(off, 0)

        @pl.when(j > 0)
        def _():
            w_wait(u)

        @pl.when(jnp.logical_and(off <= 0, off > -4))
        def _():
            pass_on(u, 1, 0)

        @pl.when(jnp.logical_and(off >= 0, off < 3))
        def _():
            pass_on(u, -1, 0)

        pass_on(u, 0, 1)
        pass_on(u, 0, -1)
        return 0

    lax.fori_loop(0, 3, first_ring, 0)
    for k in (1, 3, 2):
        slot = 2 * rem(x + k, 4) + core
        arrived(tok.at[slot], tok_recv.at[slot])
        send(tok.at[slot], tok.at[slot], tok_send, tok_recv.at[slot], at(sp, x, 1 - core))
    lax.fori_loop(3, 8, first_ring, 0)

    for k in range(4):
        slot = 2 * rem(x + k, 4) + 1 - core
        arrived(tok.at[slot], tok_recv.at[slot])

    def add_squares(s, total):
        values_in = tok[s].astype(jnp.float32)
        return total + jnp.sum(values_in * values_in, axis=1, keepdims=True)

    total_in = lax.fori_loop(0, 8, add_squares, jnp.zeros((ROWS, 1), jnp.float32))
    inv_in = lax.rsqrt(total_in / D + EPS)

    def normalize(s, _):
        gain = norm_gain[:, pl.ds(pl.multiple_of(s * 512, 512), 512)]
        rows = (tok[s].astype(jnp.float32) * inv_in * gain).astype(jnp.bfloat16)
        for j in range(8):
            nrm[s * 8 + j] = rows[:, j * UNIT : (j + 1) * UNIT]
        return 0

    lax.fori_loop(0, 8, normalize, 0)
    acc[...] = jnp.zeros_like(acc)

    def own_column(j, _):
        multiply(unit(offset(j), 0))
        return 0

    lax.fori_loop(0, 8, own_column, 0)

    def second_ring(d, plus, minus):
        def step(j, _):
            off = offset(j)
            low, high = unit(off, -d), unit(off, d)
            w_wait(low)
            if plus:
                pass_on(low, 0, 1)
            w_wait(high)
            if minus:
                pass_on(high, 0, -1)
            multiply(low)
            multiply(high)
            return 0

        return step

    lax.fori_loop(0, 8, second_ring(1, True, True), 0)
    lax.fori_loop(0, 8, second_ring(2, True, True), 0)
    lax.fori_loop(0, 4, second_ring(3, True, False), 0)
    lax.fori_loop(4, 8, second_ring(3, False, True), 0)

    def farthest(j, _):
        u = unit(offset(j), 4)
        w_wait(u)
        multiply(u)
        return 0

    lax.fori_loop(0, 8, farthest, 0)

    for m in range(2):
        keys[z, m] = acc[:, m * DK : (m + 1) * DK].astype(jnp.bfloat16)
        queries[y, m] = acc[:, 512 + m * DK : 512 + (m + 1) * DK].astype(jnp.bfloat16)
    values[z] = acc[:, 256:512].astype(jnp.bfloat16)

    def k_move(p, d):
        send(keys.at[p], keys.at[p], k_send, k_recv.at[p], at(along_z(d)))

    def v_move(p, d):
        send(values.at[p], values.at[p], v_send, v_recv.at[p], at(along_z(d)))

    def q_move(p, m, d):
        send(queries.at[p, m], queries.at[p, m], q_send, q_recv.at[p, m], at(along_y(d)))

    for d in (1, -1):
        k_move(z, d)
        for m in range(2):
            q_move(y, m, d)
        v_move(z, d)

    conv_in = acc[:, 768:896].astype(jnp.bfloat16).astype(jnp.float32)
    conv_c = acc[:, 1024:1152].astype(jnp.bfloat16).astype(jnp.float32)
    mixed[...] = (conv_c * conv_in).astype(jnp.bfloat16)
    send(mixed.at[pl.ds(176, 16)], halo, halo_send, halo_recv, at(after))

    for d in (1, 2, 3):
        low_z, high_z = rem(z - d + NZ, NZ), rem(z + d, NZ)
        low_y, high_y = rem(y - d + NY, NY), rem(y + d, NY)
        arrived(keys.at[low_z], k_recv.at[low_z])
        k_move(low_z, 1)
        arrived(keys.at[high_z], k_recv.at[high_z])
        if d < 3:
            k_move(high_z, -1)
        for m in range(2):
            arrived(queries.at[low_y, m], q_recv.at[low_y, m])
            if d < 4 - m:
                q_move(low_y, m, 1)
            arrived(queries.at[high_y, m], q_recv.at[high_y, m])
            if d < 3 + m:
                q_move(high_y, m, -1)
        arrived(values.at[low_z], v_recv.at[low_z])
        if d < 3:
            v_move(low_z, 1)
        arrived(values.at[high_z], v_recv.at[high_z])
        v_move(high_z, -1)

    arrived(halo, halo_recv)
    conv_b = acc[:, 896:1024].astype(jnp.bfloat16).astype(jnp.float32)
    mixed_now = mixed[...].astype(jnp.float32)
    earlier = jnp.where(sp > 0, halo[...].astype(jnp.float32), 0.0)
    padded = jnp.concatenate([earlier[8:16], mixed_now], axis=0)
    convolved = (
        conv_taps[0:1] * padded[6 : 6 + ROWS]
        + conv_taps[1:2] * padded[7 : 7 + ROWS]
        + conv_taps[2:3] * mixed_now
    )
    conv_out[...] = conv_b * convolved

    far_z, far_y = rem(z + 4, NZ), rem(y + 4, NY)
    for m in range(2):
        arrived(queries.at[far_y, m], q_recv.at[far_y, m])
    arrived(keys.at[far_z], k_recv.at[far_z])
    arrived(values.at[far_z], v_recv.at[far_z])

    scale = DK**-0.5 * LOG2E
    keys_here = NZ * ROWS
    spot = lax.broadcasted_iota(jnp.int32, (1, keys_here), 1)
    spot_z = div(spot, ROWS)
    key_block = spot_z * (NY * 3) + y * 3 + div(spot - spot_z * ROWS, UNIT)

    def partial(q_pos, m):
        all_keys = keys[:, m].reshape(keys_here, DK)
        all_values = values[...].reshape(keys_here, DV)
        reads, sums = [], []
        for b in range(3):
            limit = z * (NY * 3) + q_pos * 3 + b
            bias = jnp.where(key_block <= limit, 0.0, MASKED)
            scores = (
                lax.dot_general(
                    queries[q_pos, m, b * UNIT : (b + 1) * UNIT],
                    all_keys,
                    (((1,), (1,)), ((), ())),
                    preferred_element_type=jnp.float32,
                )
                + bias
            )
            top = jnp.max(scores, axis=1, keepdims=True)
            weights = jnp.exp2((scores - top) * scale)
            denom = jnp.sum(weights, axis=1, keepdims=True)
            product = jnp.dot(
                weights.astype(jnp.bfloat16), all_values, preferred_element_type=jnp.float32
            )
            reads.append(product / denom)
            level = top * scale + jnp.log2(denom)
            sums.append(jnp.where(y * 3 <= limit, level, MASKED))
        return jnp.concatenate(reads, axis=0), jnp.concatenate(sums, axis=0)

    def merge(reads, level, other, other_level):
        top = jnp.maximum(level, other_level)
        a = jnp.exp2(level - top)
        b = jnp.exp2(other_level - top)
        both = a + b
        inv = 1.0 / both
        return reads * (a * inv) + other * (b * inv), top + jnp.log2(both)

    def incoming(slot):
        arrived(in_slots.at[slot], o_recv.at[slot])
        arrived(in_rows.at[slot], l_recv.at[slot])

    def piece(t, _):
        i = div(t, 2)
        m = rem(t, 2)
        far = 4 - div(i + 1, 2)
        plus = jnp.where(jnp.logical_or(rem(i, 2) == 1, t == 0), 1, 0)
        q_pos = rem(y + far * (2 * plus - 1) + NY, NY)
        reads, level = partial(q_pos, m)
        has_other = jnp.logical_or(t >= 6, jnp.logical_or(t == 2, t == 5))

        @pl.when(has_other)
        def _():
            incoming(t)
            merged, merged_level = merge(
                reads,
                level,
                in_slots[t].astype(jnp.float32),
                to_column(in_rows[t, 0:1]),
            )
            out_slots[t] = merged.astype(jnp.bfloat16)
            out_rows[t] = to_row(merged_level)

        @pl.when(jnp.logical_not(has_other))
        def _():
            out_slots[t] = reads.astype(jnp.bfloat16)
            out_rows[t] = to_row(level)

        target = 2 * (10 - 2 * far - plus) + m
        device = at(along_y(2 * plus - 1))
        send(out_rows.at[t], in_rows.at[target], l_send, l_recv.at[target], device)
        send(out_slots.at[t], in_slots.at[target], o_send, o_recv.at[target], device)
        return 0

    lax.fori_loop(0, 14, piece, 0)

    def last_piece(m, _):
        reads, level = partial(y, m)
        for slot in (14 + m, 16 + m):
            incoming(slot)
            reads, level = merge(
                reads,
                level,
                in_slots[slot].astype(jnp.float32),
                to_column(in_rows[slot, 0:1]),
            )
        read[m] = reads
        return 0

    lax.fori_loop(0, 2, last_piece, 0)

    difference = read[0] - lam[0] * read[1]
    attn = (
        difference
        * lax.rsqrt(jnp.mean(difference * difference, axis=1, keepdims=True) + EPS)
        * head_scale[...]
    )
    conv = conv_out[...]
    both = jnp.sum(conv * conv, axis=1, keepdims=True) + jnp.sum(
        attn * attn, axis=1, keepdims=True
    )
    squares[mine] = to_row(both)
    for k in range(1, 8):
        other = rem(mine + k, 8)
        send(
            squares.at[mine],
            squares.at[mine],
            s_send,
            s_recv.at[mine],
            (sp, div(other, 2), rem(other, 2)),
        )
    for k in range(1, 8):
        other = rem(mine + k, 8)
        arrived(squares.at[other], s_recv.at[other])
    total = squares[0]
    for k in range(1, 8):
        total = total + squares[k]
    inv_rms = to_column(lax.rsqrt(total[0:1] / (CH + HEADS * DV) + EPS))
    conv_ref[...] = conv * inv_rms * gain_conv[...]
    attn_ref[...] = attn * inv_rms * gain_attn[...]

    arrived(tok.at[pl.ds(0, 7)], tok_send)
    arrived(wts.at[pl.ds(0, 63)], w_send)
    arrived(keys.at[pl.ds(0, 7)], k_send)
    arrived(values.at[pl.ds(0, 7)], v_send)
    arrived(queries.at[pl.ds(0, 7)], q_send)
    arrived(halo, halo_send)
    arrived(out_slots, o_send)
    arrived(out_rows, l_send)
    arrived(squares.at[pl.ds(0, 7)], s_send)


def local(
    tokens,
    norm_gain,
    w_conv_in,
    w_conv_b,
    w_conv_c,
    conv_taps,
    w_query,
    w_key,
    w_value,
    lam,
    head_scale,
    gain_conv,
    gain_attn,
):
    hbm = pl.BlockSpec(memory_space=pltpu.HBM)
    vmem = pl.BlockSpec(memory_space=pltpu.VMEM)
    smem = pl.BlockSpec(memory_space=pltpu.SMEM)
    bf16, f32 = jnp.bfloat16, jnp.float32
    dma = pltpu.SemaphoreType.DMA
    return pl.pallas_call(
        kernel,
        out_shape=(
            jax.ShapeDtypeStruct((ROWS, 128), f32),
            jax.ShapeDtypeStruct((ROWS, DV), f32),
        ),
        in_specs=[hbm] * 7 + [vmem, vmem, smem, vmem, vmem, vmem],
        out_specs=(vmem, vmem),
        scratch_shapes=[
            pltpu.VMEM((8, ROWS, 512), bf16),
            pltpu.VMEM((64, UNIT, COLS), bf16),
            pltpu.VMEM((64, ROWS, UNIT), bf16),
            pltpu.VMEM((ROWS, COLS), f32),
            pltpu.VMEM((NZ, 2, ROWS, DK), bf16),
            pltpu.VMEM((NZ, ROWS, DV), bf16),
            pltpu.VMEM((NY, 2, ROWS, DK), bf16),
            pltpu.VMEM((ROWS, 128), bf16),
            pltpu.VMEM((16, 128), bf16),
            pltpu.VMEM((14, ROWS, DV), bf16),
            pltpu.VMEM((14, 8, ROWS), f32),
            pltpu.VMEM((18, ROWS, DV), bf16),
            pltpu.VMEM((18, 8, ROWS), f32),
            pltpu.VMEM((8, 8, ROWS), f32),
            pltpu.VMEM((ROWS, 128), f32),
            pltpu.VMEM((2, ROWS, DV), f32),
            dma((7,)),
            dma,
            dma((8,)),
            dma,
            dma((64,)),
            dma,
            dma((NZ,)),
            dma,
            dma((NZ,)),
            dma,
            dma((NY, 2)),
            dma,
            dma,
            dma,
            dma((18,)),
            dma,
            dma((18,)),
            dma,
            dma((8,)),
        ],
        compiler_params=pltpu.CompilerParams(collective_id=0, has_side_effects=True),
    )(
        tokens,
        w_key,
        w_value,
        w_query,
        w_conv_in,
        w_conv_b,
        w_conv_c,
        norm_gain.reshape(1, D),
        conv_taps,
        lam,
        head_scale,
        gain_conv.reshape(1, -1),
        gain_attn.reshape(1, -1),
    )


def solution(mesh):
    in_specs = (
        P("sp", ("fs", "tp")),
        P(),
        P("sp", ("fs", "tp")),
        P("sp", ("fs", "tp")),
        P("sp", ("fs", "tp")),
        P(None, ("fs", "tp")),
        P("sp", ("fs", "tp")),
        P("sp", ("fs", "tp")),
        P("sp", ("fs", "tp")),
        P(("fs", "tp")),
        P(("fs", "tp"), None),
        P(("fs", "tp")),
        P(("fs", "tp")),
    )
    out_specs = (P("sp", ("fs", "tp")), P("sp", ("fs", "tp")))
    return jax.shard_map(local, mesh=mesh, in_specs=in_specs, out_specs=out_specs, check_vma=False)
```

```python
import functools
import math

import jax
import jax.numpy as jnp
from jax import lax
from jax.experimental import pallas as pl
from jax.experimental.pallas import tpu as pltpu
from jax.sharding import PartitionSpec as P

NY = 8
NZ = 8
D = 4096
CH = 1024
HEADS = 8
DK = 128
DV = 256
ROWS = 192
UNIT = 64
EPS = 1e-06
MASKED = -1e30
LOG2E = 1.4426950408889634
LN2 = 0.6931471805599453
MESH = pl.DeviceIdType.MESH

GROUP = 384


def rem(a, n):
    return lax.rem(a, jnp.int32(n))


def div(a, n):
    return lax.div(a, jnp.int32(n))


def to_row(column):
    wide = jnp.broadcast_to(column, (ROWS, 128))
    return jnp.transpose(wide)[0:8]


def to_column(row):
    tall = jnp.broadcast_to(row, (128, ROWS))
    return jnp.transpose(tall)[:, 0:1]


def kernel(
    tokens,
    w_key,
    w_value,
    w_query,
    w_conv_in,
    w_conv_b,
    w_conv_c,
    norm_gain,
    conv_taps,
    lam,
    head_scale,
    gain_conv,
    gain_attn,
    conv_ref,
    attn_ref,
    tok,
    wts,
    nrm,
    acc,
    keys,
    values,
    queries,
    mixed,
    halo,
    out_slots,
    out_rows,
    in_slots,
    in_rows,
    squares,
    conv_out,
    turned,
    held_reads,
    held_levels,
    local_sem,
    tok_send,
    tok_recv,
    far_recv,
    w_send,
    w_recv,
    k_send,
    k_recv,
    v_send,
    v_recv,
    q_send,
    q_recv,
    halo_send,
    halo_recv,
    o_send,
    o_recv,
    l_send,
    l_recv,
    s_send,
    s_recv,
):
    sp = lax.axis_index("sp")
    x = lax.axis_index("fs")
    core = lax.axis_index("tp")
    y = rem(sp, NY)
    z = div(sp, NY)
    mine = 2 * x + core

    def at(s, f=x, t=core):
        return (s, f, t)

    def along_y(d):
        return sp + rem(y + d + NY, NY) - y

    def along_z(d):
        return sp + (rem(z + d + NZ, NZ) - z) * NY

    def send(src, dst, send_sem, recv_sem, device):
        pltpu.make_async_remote_copy(
            src_ref=src,
            dst_ref=dst,
            send_sem=send_sem,
            recv_sem=recv_sem,
            device_id=device,
            device_id_type=MESH,
        ).start()

    def arrived(ref, sem):
        pltpu.make_async_copy(ref, ref, sem).wait()

    own = [
        pltpu.make_async_copy(tokens, tok.at[mine], local_sem.at[0]),
    ]
    group_parts = (
        (w_key, 0, 0, 0, 256),
        (w_query, 0, 0, 256, 128),
        (w_value, 0, 1, 0, 256),
        (w_query, 128, 1, 256, 128),
        (w_conv_in, 0, 2, 0, 128),
        (w_conv_b, 0, 2, 128, 128),
        (w_conv_c, 0, 2, 256, 128),
    )
    home = y * (1 + 7 * core) + z * (8 - 7 * core)
    for k, (w, start, g, column, width) in enumerate(group_parts):
        own.append(
            pltpu.make_async_copy(
                w.at[:, pl.ds(start, width)],
                wts.at[g, home, :, pl.ds(column, width)],
                local_sem.at[1 + k],
            )
        )
    for copy in own:
        copy.start()

    barrier = pltpu.get_barrier_semaphore()

    def greet(device):
        pl.semaphore_signal(barrier, inc=1, device_id=device, device_id_type=MESH)

    for d in (1, -1):
        greet(at(along_y(d)))
        greet(at(along_z(d)))
    for k in range(1, 8):
        other = rem(mine + k, 8)
        greet((sp, div(other, 2), rem(other, 2)))
    before = rem(sp + NY * NZ - 1, NY * NZ)
    after = rem(sp + 1, NY * NZ)
    greet(at(before))
    for copy in own:
        copy.wait()
    pl.semaphore_wait(barrier, 12)

    def slot_at(k):
        return 2 * rem(x + k + 4, 4) + core

    def tok_to(k, slot, rows, sem):
        part = tok.at[slot, rows]
        send(part, part, tok_send, sem, at(sp, rem(x + k + 4, 4)))

    def to_partner(slot):
        send(tok.at[slot], tok.at[slot], tok_send, tok_recv.at[slot], at(sp, x, 1 - core))

    upper, lower = pl.ds(0, ROWS // 2), pl.ds(ROWS // 2, ROWS // 2)
    for k in (1, -1):
        tok_to(k, mine, pl.ds(0, ROWS), tok_recv.at[mine])
    to_partner(mine)

    stride1 = 1 + 7 * core
    stride2 = 8 - 7 * core
    pos1 = rem(lax.div(sp, stride1), 8)
    pos2 = rem(lax.div(sp, stride2), 8)

    def place(d1, d2):
        return rem(pos2 + d2 + 8, 8) * 8 + rem(pos1 + d1 + 8, 8)

    def device(d1, d2):
        return at(rem(pos1 + d1 + 8, 8) * stride1 + rem(pos2 + d2 + 8, 8) * stride2)

    def pass_on(g, u, d1, d2):
        send(wts.at[g, u], wts.at[g, u], w_send.at[g], w_recv.at[g, u], device(d1, d2))

    def w_wait(g, u):
        arrived(wts.at[g, u], w_recv.at[g, u])

    def offset(j):
        return div(j + 1, 2) * (1 - 2 * rem(j, 2))

    def loop(first, last, *steps):
        def body(j, _):
            for step in steps:
                step(j)
            return 0

        lax.fori_loop(first, last, body, 0)

    def first_ring(g, lag=0, onward=True):
        def step(i):
            j = i - lag
            off = offset(j)
            u = place(off, 0)

            @pl.when(j > 0)
            def _():
                w_wait(g, u)

            @pl.when(jnp.logical_and(off <= 0, off > -4))
            def _():
                pass_on(g, u, 1, 0)

            @pl.when(jnp.logical_and(off >= 0, off < 3))
            def _():
                pass_on(g, u, -1, 0)

            if onward:
                across(g)(j)

        return step

    def across(g):
        def step(j):
            u = place(offset(j), 0)
            pass_on(g, u, 0, 1)
            pass_on(g, u, 0, -1)

        return step

    def second_ring(g, d, lag=0):
        def step(i):
            j = i - lag
            off = offset(j)
            if d == 4:
                w_wait(g, place(off, 4))
                return
            low, high = place(off, -d), place(off, d)
            w_wait(g, low)
            if d < 3:
                pass_on(g, low, 0, 1)
            else:

                @pl.when(j < 4)
                def _():
                    pass_on(g, low, 0, 1)

            w_wait(g, high)
            if d < 3:
                pass_on(g, high, 0, -1)
            else:

                @pl.when(j >= 4)
                def _():
                    pass_on(g, high, 0, -1)

        return step

    def multiply(*distances):
        for d in distances:
            p = rem(pos2 + d + 8, 8)
            for g in range(2):
                block = wts[g, pl.ds(p * 8, 8)].reshape(8 * UNIT, GROUP)
                acc[g] += jnp.dot(nrm[p], block, preferred_element_type=jnp.float32)

    with jax.named_scope("ring1a"):
        loop(0, 3, first_ring(0), first_ring(1))
    with jax.named_scope("tokpass"):
        for k, rows in ((-1, upper), (1, lower)):
            slot = slot_at(k)
            arrived(tok.at[slot], tok_recv.at[slot])
            tok_to(-k, slot, rows, far_recv.at[0 if k < 0 else 1])
            to_partner(slot)
    with jax.named_scope("ring1b"):
        loop(
            3,
            8,
            first_ring(0),
            first_ring(1),
            second_ring(0, 1, 3),
            second_ring(1, 1, 3),
            first_ring(2, 3, False),
        )

    with jax.named_scope("tokpass2"):
        far = slot_at(2)
        arrived(tok.at[far, upper], far_recv.at[0])
        arrived(tok.at[far, lower], far_recv.at[1])
        to_partner(far)
    with jax.named_scope("ring1c"):
        loop(5, 8, second_ring(0, 1), second_ring(1, 1), first_ring(2, 0, False))
    with jax.named_scope("norm"):
        for k in range(4):
            slot = 2 * rem(x + k, 4) + 1 - core
            arrived(tok.at[slot], tok_recv.at[slot])

        def add_squares(s, total):
            values_in = tok[s].astype(jnp.float32)
            return total + jnp.sum(values_in * values_in, axis=1, keepdims=True)

        total_in = lax.fori_loop(0, 8, add_squares, jnp.zeros((ROWS, 1), jnp.float32))
        inv_in = lax.rsqrt(total_in / D + EPS)

        def normed(s):
            gain = norm_gain[:, s * 512 : (s + 1) * 512]
            return (tok[s].astype(jnp.float32) * inv_in * gain).astype(jnp.bfloat16)

        @pl.when(core == 0)
        def _():
            for s in range(8):
                nrm[s] = normed(s)

        @pl.when(core == 1)
        def _():
            for s in range(8):
                rows = normed(s)
                for j in range(8):
                    nrm[j, :, s * UNIT : (s + 1) * UNIT] = rows[:, j * UNIT : (j + 1) * UNIT]

        acc[...] = jnp.zeros_like(acc)
        multiply(0, -1, 1)
    with jax.named_scope("d2"):
        loop(0, 8, second_ring(0, 2), second_ring(1, 2))
        multiply(-2, 2)
    with jax.named_scope("d3"):
        loop(0, 8, second_ring(0, 3), second_ring(1, 3))
        loop(0, 8, across(2))
        multiply(-3, 3)
    with jax.named_scope("d4"):
        loop(0, 8, second_ring(0, 4), second_ring(1, 4))
        multiply(4)

    with jax.named_scope("qkv"):
        for m in range(2):
            keys[z, m] = acc[0, :, m * DK : (m + 1) * DK].astype(jnp.bfloat16)
            queries[y, m] = acc[m, :, 256:384].astype(jnp.bfloat16)
        values[z] = acc[1, :, 0:256].astype(jnp.bfloat16)

    def k_move(p, d):
        send(keys.at[p], keys.at[p], k_send, k_recv.at[p], at(along_z(d)))

    def v_move(p, d):
        send(values.at[p], values.at[p], v_send, v_recv.at[p], at(along_z(d)))

    def q_move(p, m, d):
        send(queries.at[p, m], queries.at[p, m], q_send, q_recv.at[p, m], at(along_y(d)))

    for d in (1, -1):
        k_move(z, d)
        for m in range(2):
            q_move(y, m, d)
        v_move(z, d)

    for d in (1, 2, 3):
        with jax.named_scope(f"qkv{d}"):
            low_z, high_z = rem(z - d + NZ, NZ), rem(z + d, NZ)
            low_y, high_y = rem(y - d + NY, NY), rem(y + d, NY)
            arrived(keys.at[low_z], k_recv.at[low_z])
            k_move(low_z, 1)
            arrived(keys.at[high_z], k_recv.at[high_z])
            if d < 3:
                k_move(high_z, -1)
            for m in range(2):
                arrived(queries.at[low_y, m], q_recv.at[low_y, m])
                if d < 4 - m:
                    q_move(low_y, m, 1)
                arrived(queries.at[high_y, m], q_recv.at[high_y, m])
                if d < 3 + m:
                    q_move(high_y, m, -1)
            arrived(values.at[low_z], v_recv.at[low_z])
            if d < 3:
                v_move(low_z, 1)
            arrived(values.at[high_z], v_recv.at[high_z])
            v_move(high_z, -1)
        with jax.named_scope(f"w{d}"):
            if d == 1:
                loop(0, 4, second_ring(2, 1))
            if d == 2:
                loop(4, 8, second_ring(2, 1))
            if d == 3:
                loop(0, 4, second_ring(2, 2))

    with jax.named_scope("qkv4"):
        far_z, far_y = rem(z + 4, NZ), rem(y + 4, NY)
        for m in range(2):
            arrived(queries.at[far_y, m], q_recv.at[far_y, m])
        arrived(keys.at[far_z], k_recv.at[far_z])
        arrived(values.at[far_z], v_recv.at[far_z])

    keys_here = NZ * ROWS
    with jax.named_scope("turn"):
        for m in range(2):
            turned[m] = jnp.transpose(keys[:, m].reshape(keys_here, DK))

    def convolution_input():
        every = wts[2].reshape(D, GROUP)
        acc[2] = jnp.zeros((ROWS, GROUP), jnp.float32)
        for p in range(8):
            acc[2] += jnp.dot(
                nrm[p],
                every[p * 512 : (p + 1) * 512],
                preferred_element_type=jnp.float32,
            )
        conv_in = acc[2, :, 0:128].astype(jnp.bfloat16).astype(jnp.float32)
        conv_c = acc[2, :, 256:384].astype(jnp.bfloat16).astype(jnp.float32)
        mixed[...] = (conv_c * conv_in).astype(jnp.bfloat16)
        send(mixed.at[pl.ds(176, 16)], halo, halo_send, halo_recv, at(after))

    def convolution():
        arrived(halo, halo_recv)
        conv_b = acc[2, :, 128:256].astype(jnp.bfloat16).astype(jnp.float32)
        mixed_now = mixed[...].astype(jnp.float32)
        earlier = jnp.where(sp > 0, halo[...].astype(jnp.float32), 0.0)
        padded = jnp.concatenate([earlier[8:16], mixed_now], axis=0)
        convolved = (
            conv_taps[0:1] * padded[6 : 6 + ROWS]
            + conv_taps[1:2] * padded[7 : 7 + ROWS]
            + conv_taps[2:3] * mixed_now
        )
        conv_out[...] = conv_b * convolved

    scale = DK**-0.5 * LOG2E
    spot = lax.broadcasted_iota(jnp.int32, (1, keys_here), 1)
    spot_z = div(spot, ROWS)
    key_block = spot_z * (NY * 3) + y * 3 + div(spot - spot_z * ROWS, UNIT)

    def partials(q_pos):
        first = z * (NY * 3) + q_pos * 3
        biases = [jnp.where(key_block <= first + b, 0.0, MASKED) for b in range(3)]
        weights, denoms, levels = [], [], []
        for m in range(2):
            scores = jnp.dot(
                queries[q_pos, m], turned[m], preferred_element_type=jnp.float32
            )
            for b in range(3):
                part = scores[b * UNIT : (b + 1) * UNIT] + biases[b]
                top = jnp.max(part, axis=1, keepdims=True)
                shares = jnp.exp2((part - top) * scale)
                denom = jnp.sum(shares, axis=1, keepdims=True)
                weights.append(shares.astype(jnp.bfloat16))
                denoms.append(denom)
                level = top * scale + jnp.log2(denom)
                levels.append(jnp.where(y * 3 <= first + b, level, MASKED))
        product = jnp.dot(
            jnp.concatenate(weights, axis=0),
            values[...].reshape(keys_here, DV),
            preferred_element_type=jnp.float32,
        ) * (1.0 / jnp.concatenate(denoms, axis=0))
        level = jnp.concatenate(levels, axis=0)
        return [(product[m * ROWS : (m + 1) * ROWS], level[m * ROWS : (m + 1) * ROWS]) for m in range(2)]

    def merge(reads, level, other, other_level):
        top = jnp.maximum(level, other_level)
        a = jnp.exp2(level - top)
        b = jnp.exp2(other_level - top)
        both = a + b
        inv = 1.0 / both
        return reads * (a * inv) + other * (b * inv), top + jnp.log2(both)

    def incoming(slot):
        arrived(in_slots.at[slot], o_recv.at[slot])
        arrived(in_rows.at[slot], l_recv.at[slot])

    def pieces(i, _):
        hops = 4 - div(i + 1, 2)
        q_pos = rem(y + hops * (2 * rem(i, 2) - 1) + NY, NY)
        with jax.named_scope("partial"):
            both = partials(q_pos)

        def post(t, m, reads, level):
            out_slots[t] = reads.astype(jnp.bfloat16)
            out_rows[t] = to_row(level)
            step = div(t, 2)
            hop = 4 - div(step + 1, 2)
            plus = jnp.where(step == 0, 1 - m, rem(step, 2))
            target = 2 * (10 - 2 * hop - plus) + m
            to = at(along_y(2 * plus - 1))
            send(out_rows.at[t], in_rows.at[target], l_send, l_recv.at[target], to)
            send(out_slots.at[t], in_slots.at[target], o_send, o_recv.at[target], to)

        def join(t, m, reads, level):
            with jax.named_scope("incoming"):
                incoming(t)
            post(
                t,
                m,
                *merge(reads, level, in_slots[t].astype(jnp.float32), to_column(in_rows[t, 0:1])),
            )

        for m in range(2):
            reads, level = both[m]

            @pl.when(i >= 3)
            def _():
                join(2 * i + m, m, reads, level)

            @pl.when(i == 1 + m)
            def _():
                held_reads[m] = reads
                held_levels[m] = jnp.broadcast_to(level, (ROWS, 128))

            @pl.when(jnp.logical_and(i < 3, i != 1 + m))
            def _():
                post(2 * i + m, m, reads, level)

        @pl.when(i == 2)
        def _():
            join(2, 0, held_reads[0], held_levels[0, :, 0:1])
            join(5, 1, held_reads[1], held_levels[1, :, 0:1])

        with jax.named_scope("weights"):

            @pl.when(i == 0)
            def _():
                loop(4, 8, second_ring(2, 2))

            @pl.when(i == 1)
            def _():
                loop(0, 4, second_ring(2, 3))

            @pl.when(i == 2)
            def _():
                loop(4, 8, second_ring(2, 3))

            @pl.when(i == 3)
            def _():
                loop(0, 4, second_ring(2, 4))

            @pl.when(i == 4)
            def _():
                loop(4, 8, second_ring(2, 4))

            @pl.when(i == 5)
            def _():
                convolution_input()

        return 0

    with jax.named_scope("pieces"):
        lax.fori_loop(0, 7, pieces, 0)

    with jax.named_scope("last"):
        own_parts = partials(y)
        read = []
        for m in range(2):
            reads, level = own_parts[m]
            for slot in (14 + m, 16 + m):
                with jax.named_scope("incoming"):
                    incoming(slot)
                reads, level = merge(
                    reads,
                    level,
                    in_slots[slot].astype(jnp.float32),
                    to_column(in_rows[slot, 0:1]),
                )
            read.append(reads)

    def finish():
        arrived(tok.at[pl.ds(0, 7)], tok_send)
        for g in range(3):
            arrived(wts.at[g, pl.ds(0, 63)], w_send.at[g])
        arrived(keys.at[pl.ds(0, 7)], k_send)
        arrived(values.at[pl.ds(0, 7)], v_send)
        arrived(queries.at[pl.ds(0, 7)], q_send)
        arrived(halo, halo_send)
        arrived(out_slots, o_send)
        arrived(out_rows, l_send)
        arrived(squares.at[pl.ds(0, 7)], s_send)

    with jax.named_scope("conv"):
        convolution()
    with jax.named_scope("sum"):
        difference = read[0] - lam[0] * read[1]
        attn = (
            difference
            * lax.rsqrt(jnp.mean(difference * difference, axis=1, keepdims=True) + EPS)
            * head_scale[...]
        )
        conv = conv_out[...]
        both = jnp.sum(conv * conv, axis=1, keepdims=True) + jnp.sum(
            attn * attn, axis=1, keepdims=True
        )
        squares[mine] = to_row(both)
        for k in range(1, 8):
            other = rem(mine + k, 8)
            send(
                squares.at[mine],
                squares.at[mine],
                s_send,
                s_recv.at[mine],
                (sp, div(other, 2), rem(other, 2)),
            )
    with jax.named_scope("exchange"):
        for k in range(1, 8):
            other = rem(mine + k, 8)
            arrived(squares.at[other], s_recv.at[other])
    with jax.named_scope("out"):
        total = squares[0]
        for k in range(1, 8):
            total = total + squares[k]
        inv_rms = to_column(lax.rsqrt(total[0:1] / (CH + HEADS * DV) + EPS))
        conv_ref[...] = conv * inv_rms * gain_conv[...]
        attn_ref[...] = attn * inv_rms * gain_attn[...]

    with jax.named_scope("drain"):
        finish()


def local(
    tokens,
    norm_gain,
    w_conv_in,
    w_conv_b,
    w_conv_c,
    conv_taps,
    w_query,
    w_key,
    w_value,
    lam,
    head_scale,
    gain_conv,
    gain_attn,
):
    hbm = pl.BlockSpec(memory_space=pltpu.HBM)
    vmem = pl.BlockSpec(memory_space=pltpu.VMEM)
    smem = pl.BlockSpec(memory_space=pltpu.SMEM)
    bf16, f32 = jnp.bfloat16, jnp.float32
    dma = pltpu.SemaphoreType.DMA
    return pl.pallas_call(
        kernel,
        out_shape=(
            jax.ShapeDtypeStruct((ROWS, 128), f32),
            jax.ShapeDtypeStruct((ROWS, DV), f32),
        ),
        in_specs=[hbm] * 7 + [vmem, vmem, smem, vmem, vmem, vmem],
        out_specs=(vmem, vmem),
        scratch_shapes=[
            pltpu.VMEM((8, ROWS, 512), bf16),
            pltpu.VMEM((3, 64, UNIT, GROUP), bf16),
            pltpu.VMEM((8, ROWS, 512), bf16),
            pltpu.VMEM((3, ROWS, GROUP), f32),
            pltpu.VMEM((NZ, 2, ROWS, DK), bf16),
            pltpu.VMEM((NZ, ROWS, DV), bf16),
            pltpu.VMEM((NY, 2, ROWS, DK), bf16),
            pltpu.VMEM((ROWS, 128), bf16),
            pltpu.VMEM((16, 128), bf16),
            pltpu.VMEM((14, ROWS, DV), bf16),
            pltpu.VMEM((14, 8, ROWS), f32),
            pltpu.VMEM((18, ROWS, DV), bf16),
            pltpu.VMEM((18, 8, ROWS), f32),
            pltpu.VMEM((8, 8, ROWS), f32),
            pltpu.VMEM((ROWS, 128), f32),
            pltpu.VMEM((2, DK, NZ * ROWS), bf16),
            pltpu.VMEM((2, ROWS, DV), f32),
            pltpu.VMEM((2, ROWS, 128), f32),
            dma((8,)),
            dma,
            dma((8,)),
            dma((2,)),
            dma((3,)),
            dma((3, 64)),
            dma,
            dma((NZ,)),
            dma,
            dma((NZ,)),
            dma,
            dma((NY, 2)),
            dma,
            dma,
            dma,
            dma((18,)),
            dma,
            dma((18,)),
            dma,
            dma((8,)),
        ],
        compiler_params=pltpu.CompilerParams(collective_id=0, has_side_effects=True),
    )(
        tokens,
        w_key,
        w_value,
        w_query,
        w_conv_in,
        w_conv_b,
        w_conv_c,
        norm_gain.reshape(1, D),
        conv_taps,
        lam,
        head_scale,
        gain_conv.reshape(1, -1),
        gain_attn.reshape(1, -1),
    )


def solution(mesh):
    in_specs = (
        P("sp", ("fs", "tp")),
        P(),
        P("sp", ("fs", "tp")),
        P("sp", ("fs", "tp")),
        P("sp", ("fs", "tp")),
        P(None, ("fs", "tp")),
        P("sp", ("fs", "tp")),
        P("sp", ("fs", "tp")),
        P("sp", ("fs", "tp")),
        P(("fs", "tp")),
        P(("fs", "tp"), None),
        P(("fs", "tp")),
        P(("fs", "tp")),
    )
    out_specs = (P("sp", ("fs", "tp")), P("sp", ("fs", "tp")))
    return jax.shard_map(local, mesh=mesh, in_specs=in_specs, out_specs=out_specs, check_vma=False)
```
